32 devices in a mesh: ep: 16 (over z, y, x), tp: 2 (over core).
Axes of the slice: x: 2, y: 2, z: 4, core: 2. Of those that a mesh axis runs over, the one named last changes fastest.
Arguments:
- tokens: bfloat16 [2048, 2048], P('ep', 'tp'), may hold values from -6 to 6
- cotangent: bfloat16 [2048, 2048], P('ep', 'tp'), may hold values from -6 to 6
- routes: int32 [2048, 2], P('ep'), may hold values from 0 to 15, all different within a row; in each aligned block of 128 rows (0 to 127, 128 to 255, ...) at most 24 rows name the same one
- route_weights: float32 [2048, 2], P('ep'), may hold values from 0.1 to 2.5
- gate_proj: bfloat16 [16, 2048, 512], P('ep', None, 'tp'), may hold values from -0.125 to 0.125
- up_proj: bfloat16 [16, 2048, 512], P('ep', None, 'tp'), may hold values from -0.125 to 0.125
- down_proj: bfloat16 [16, 512, 2048], P('ep', 'tp'), may hold values from -0.25 to 0.25
- shared_gate: bfloat16 [2048, 512], P(None, 'tp'), may hold values from -0.125 to 0.125
- shared_up: bfloat16 [2048, 512], P(None, 'tp'), may hold values from -0.125 to 0.125
- shared_down: bfloat16 [2048, 512], P(None, 'tp'), may hold values from -0.25 to 0.25
Outputs:
- token_grad: bfloat16 [2048, 2048], P('ep', 'tp')
- weight_grad: float32 [2048, 2], P('ep')
- gate_grad: bfloat16 [16, 2048, 512], P('ep', None, 'tp')
- up_grad: bfloat16 [16, 2048, 512], P('ep', None, 'tp')
- down_grad: bfloat16 [16, 512, 2048], P('ep', 'tp')
- sharedgate_grad: float32 [2048, 512], P('ep', 'tp')
- sharedup_grad: float32 [2048, 512], P('ep', 'tp')
- shareddown_grad: float32 [2048, 512], P('ep', 'tp')
The draws below stay inside these ranges and needn't reach their ends.
Inputs may be any that keep to these rules, and one draw needn't show every extreme that they name: `routes`: the 2 entries of a token name different experts. Among the 128 tokens of one group no expert is named more than 24 times, and in some groups an expert is named exactly 24 times.
All inputs are finite; a program needn't handle non-finite values.
Results may differ from the reference program's by a relative error of at most 0.007.
Values may be sent and summed in bfloat16 or wider, within the bound.
A program may use at most 128 MiB of HBM per device.

```python
import math
import jax
import jax.numpy as jnp
import numpy as np
from jax import lax

D = 2048
F = 512
FS = 512
TOP_K = 2
TOK_DEV = 128
EXPERTS = 16
TOKENS = 2048
CAP = 24
N_EP = 16
N_TP = 2


def strengthened(result, key, source, target, shards_of, factor):
    def block_of(position):
        return (jnp.arange(result.shape[position]) // (result.shape[position] // shards_of)).reshape((-1,) + (1,) * (result.ndim - 1 - position))

    one_side = jax.random.permutation(key, shards_of)[block_of(target)]
    other_side = (block_of(target) + shards_of // 2) % shards_of
    return jnp.where((block_of(source) == one_side) | (block_of(source) == other_side), factor * result, result)


def block_levels(rng, dims, pieces, smallest, high):
    def one(dim, blocks):
        steps = jax.random.uniform(jax.random.fold_in(jax.random.fold_in(rng, 6), dim), (blocks,), jnp.float32, smallest / len(pieces), high / len(pieces))
        return jnp.repeat(jnp.exp(steps), dims[dim] // blocks).reshape((-1,) + (1,) * (len(dims) - dim - 1))

    factor_of = one(*pieces[0])
    for cut in pieces[1:]:
        factor_of = factor_of * one(*cut)
    return factor_of


def deal_out(stream_key, own, number, rows, number_of, top, most, slope):
    sequence = jax.random.permutation(stream_key, number_of)
    crowded, common = portions_of(number_of, rows * top, most, slope, True), portions_of(number_of, rows * top, most, slope, False)
    places = jnp.arange(number_of)

    def named(lengths, offset_by):
        used = int((lengths > 0).sum())
        fixed = max(1, used // 4)
        moved = fixed + (places - fixed + offset_by * (used - fixed)) % max(1, number_of - fixed)
        return jnp.zeros((number_of,), jnp.int32).at[sequence[jnp.where(places < fixed, places, moved)]].set(jnp.asarray(lengths, jnp.int32))

    lengths = jnp.where(number % 4 == 0, named(crowded, number // 4), named(common, number - number // 4 - 1))
    mixed = jax.random.permutation(jax.random.fold_in(own, 3), number_of)
    source_of, taker = mixed[0:number_of // 2 * 2:2], mixed[1:number_of // 2 * 2:2]
    slack = jnp.minimum(lengths[source_of] - 1, most - lengths[taker]) // 2
    slack = jnp.where((source_of == sequence[0]) | (taker == sequence[0]) | (lengths[taker] == 0), 0, jnp.maximum(slack, 0))
    moved = jax.random.randint(jax.random.fold_in(own, 4), (number_of // 2,), 0, 1 << 20) % (slack + 1)
    lengths = lengths.at[source_of].add(-moved).at[taker].add(moved)
    members = jnp.searchsorted(jnp.cumsum(lengths), jnp.arange(rows * top), side="right").astype(jnp.int32)
    grid = members.reshape(top, rows).T
    grid = grid[jax.random.permutation(jax.random.fold_in(own, 1), rows)]
    offset_by = jax.random.randint(jax.random.fold_in(own, 2), (rows, 1), 0, top)
    return jnp.take_along_axis(grid, (jnp.arange(top)[None, :] + offset_by) % top, axis=1)


def portions_of(number_of, total, limit, skew, full):
    portions = [(1 << 20) // math.isqrt(rank ** skew) + 1 for rank in range(1, number_of + 1)]
    largest = limit if full else min(limit, max(-(-total // number_of), total * portions[0] // sum(portions)))
    least = 1 if total - largest >= number_of - 1 else 0
    given, rest = [largest] + [least] * (number_of - 1), total - largest - least * (number_of - 1)
    while rest > 0:
        movable = [i for i in range(1, number_of) if given[i] < largest] or [i for i in range(1, number_of) if given[i] < limit]
        whole, budget = sum([portions[i] for i in movable]), rest
        for i in movable:
            extra = min(limit - given[i], max(1, budget * portions[i] // whole), rest)
            given[i] = given[i] + extra
            rest = rest - extra
    return np.array(given)


def centred(key, shape, deviation, most, shards=(), kind=jnp.bfloat16):
    entries = jax.random.normal(key, shape, jnp.float32) * deviation
    if len(shards) > 0:
        entries = block_levels(key, shape, shards, -0.22, 0.18) * entries
    return jnp.clip(entries, min=-most, max=most).astype(kind)


def gaussian_with(stream_key, extent, spread, limit, shards, heavy, held_as=jnp.bfloat16):
    entries = spread * jax.random.normal(stream_key, extent, jnp.float32)
    if shards:
        entries = entries * block_levels(stream_key, extent, shards, -0.22, 0.18)
    return jnp.clip(strengthened(entries, jax.random.fold_in(stream_key, 3), *heavy), -limit, limit).astype(held_as)


def setup_inputs(seed: int = 0) -> dict:
    streams_of = jax.random.split(jax.random.key(seed), 11)
    tokens = gaussian_with(streams_of[0], (TOKENS, D), 1.0, 6.0, ((0, 16), (1, 2)), (0, 1, 16, 2.0))
    cotangent = gaussian_with(streams_of[1], (TOKENS, D), 1.0, 6.0, ((0, 16), (1, 2)), (0, 1, 16, 2.0))
    routes_keys = jax.random.split(jax.random.fold_in(streams_of[2], 1), TOKENS // TOK_DEV)
    routes_turns = jax.random.permutation(jax.random.fold_in(streams_of[2], 3), TOKENS // TOK_DEV)
    routes = jax.vmap(lambda own, number: deal_out(jax.random.fold_in(streams_of[2], 2), own, number, TOK_DEV, EXPERTS, TOP_K, CAP, 1))(routes_keys, routes_turns).reshape((TOKENS, TOP_K))
    route_weights = jnp.clip(jnp.exp(math.log(2.5) - 3.218876 * jax.random.uniform(streams_of[3], (TOKENS, TOP_K), jnp.float32) ** block_levels(streams_of[3], (TOKENS, TOP_K), ((0, 16),), -0.2, 0.2)), 0.1, 2.5)
    gate_proj = centred(streams_of[4], (EXPERTS, D, F), D ** -0.5, 0.125, ((0, 16), (2, 2)))
    up_proj = centred(streams_of[5], (EXPERTS, D, F), D ** -0.5, 0.125, ((0, 16), (2, 2)))
    down_proj = centred(streams_of[6], (EXPERTS, F, D), F ** -0.5, 0.25, ((0, 16), (1, 2)))
    shared_gate = centred(streams_of[7], (D, FS), D ** -0.5, 0.125, ((1, 2),))
    shared_up = centred(streams_of[8], (D, FS), D ** -0.5, 0.125, ((1, 2),))
    shared_down = centred(streams_of[9], (D, FS), FS ** -0.5, 0.25, ((1, 2),))
    return dict(tokens=tokens, cotangent=cotangent, routes=routes, route_weights=route_weights, gate_proj=gate_proj, up_proj=up_proj, down_proj=down_proj, shared_gate=shared_gate, shared_up=shared_up, shared_down=shared_down)


def slot_table(routes, experts, capacity):
    assigned = routes.shape[0] * routes.shape[1]
    flat_routes = routes.reshape(assigned).astype(jnp.int32)
    onehot = (flat_routes[:, None] == jnp.arange(experts, dtype=jnp.int32)[None, :]).astype(jnp.int32)
    before = jnp.cumsum(onehot, axis=0) - onehot
    slot_rank = jnp.sum(before * onehot, axis=1).astype(jnp.int32)
    slot_of = (flat_routes * capacity + slot_rank).astype(jnp.int32)
    empty = jnp.full((experts * capacity,), assigned, jnp.int32)
    slot_owner = empty.at[slot_of].set(jnp.arange(assigned, dtype=jnp.int32))
    return slot_of, slot_owner


def silu_parts(preact):
    sigmoid_v = jax.nn.sigmoid(preact)
    return preact * sigmoid_v, sigmoid_v * (1.0 + preact * (1.0 - sigmoid_v))


def rounded(partial_value):
    return lax.optimization_barrier(partial_value.astype(jnp.bfloat16)).astype(jnp.float32)


def contract_rows(left, right):
    return lax.dot_general(left, right, (((0,), (0,)), ((), ())), preferred_element_type=jnp.float32)


def contract_cols(left, right):
    return lax.dot_general(left, right, (((1,), (1,)), ((), ())), preferred_element_type=jnp.float32)


def reference(tokens, cotangent, routes, route_weights, gate_proj, up_proj, down_proj, shared_gate, shared_up, shared_down):
    assigned = TOK_DEV * TOP_K
    row_width = tokens.shape[1]
    block_size = F // N_TP
    slot_of, slot_owner = jax.vmap(lambda device_routes: slot_table(device_routes, EXPERTS, CAP))(
        routes.reshape(N_EP, TOK_DEV, TOP_K))
    filled = slot_owner < assigned
    owner_safe = jnp.minimum(slot_owner, assigned - 1)
    source = jnp.arange(N_EP, dtype=jnp.int32)[:, None]
    token_at = (source * TOK_DEV + owner_safe // TOP_K).astype(jnp.int32)
    assign_at = (source * assigned + owner_safe).astype(jnp.int32)
    flat_weights = route_weights.reshape(N_EP * assigned)
    weight_at = jnp.where(filled, flat_weights[assign_at], jnp.zeros((), jnp.float32))

    def by_expert(layout):
        return jnp.swapaxes(layout.reshape(N_EP, EXPERTS, CAP), 0, 1).reshape(EXPERTS, N_EP * CAP)

    def expert_step(running, inputs):
        input_acc, weight_acc = running
        token_index, assign_index, slot_weights, slot_live, gate_mat, up_mat, down_mat = inputs
        slot_rows = jnp.where(slot_live[:, None], tokens[token_index], jnp.zeros((), jnp.bfloat16))
        slot_cot = (slot_weights[:, None] * cotangent[token_index].astype(jnp.float32)).astype(jnp.bfloat16)
        gate_pre = jnp.dot(slot_rows, gate_mat, preferred_element_type=jnp.float32)
        up_pre = jnp.dot(slot_rows, up_mat, preferred_element_type=jnp.float32)
        gate_act, gate_slope = silu_parts(gate_pre)
        hidden = gate_act * up_pre
        back_grad = contract_cols(slot_cot, down_mat)
        hidden_low = hidden.astype(jnp.bfloat16)
        down_grad = contract_rows(hidden_low, slot_cot).astype(jnp.bfloat16)
        gate_delta = (back_grad * up_pre * gate_slope).astype(jnp.bfloat16)
        up_delta = (back_grad * gate_act).astype(jnp.bfloat16)
        gate_grad = contract_rows(slot_rows, gate_delta).astype(jnp.bfloat16)
        up_grad = contract_rows(slot_rows, up_delta).astype(jnp.bfloat16)
        slot_sum = jnp.zeros((slot_rows.shape[0], row_width), jnp.float32)
        product_sum = jnp.zeros((slot_rows.shape[0],), jnp.float32)
        for block_index in range(N_TP):
            start_col = block_index * block_size
            stop_col = start_col + block_size
            partial_value = contract_cols(gate_delta[:, start_col:stop_col], gate_mat[:, start_col:stop_col])
            partial_value = partial_value + contract_cols(up_delta[:, start_col:stop_col], up_mat[:, start_col:stop_col])
            slot_sum = slot_sum + rounded(partial_value)
            product_sum = product_sum + rounded(jnp.sum(hidden[:, start_col:stop_col] * back_grad[:, start_col:stop_col], axis=1))
        slot_low = rounded(slot_sum)
        product_low = rounded(product_sum)
        input_acc = input_acc.at[token_index].add(jnp.where(slot_live[:, None], slot_low, jnp.zeros((), jnp.float32)))
        weight_acc = weight_acc.at[assign_index].add(jnp.where(slot_live, product_low, jnp.zeros((), jnp.float32)))
        return (input_acc, weight_acc), (gate_grad, up_grad, down_grad)

    start_acc = (jnp.zeros((TOKENS, row_width), jnp.float32), jnp.zeros((TOKENS * TOP_K,), jnp.float32))
    (input_acc, weight_acc), (gate_grad, up_grad, down_grad) = lax.scan(
        expert_step, start_acc,
        (by_expert(token_at), by_expert(assign_at), by_expert(weight_at), by_expert(filled), gate_proj, up_proj, down_proj))

    mix_gate = jnp.dot(tokens, shared_gate, preferred_element_type=jnp.float32)
    mix_up = jnp.dot(tokens, shared_up, preferred_element_type=jnp.float32)
    mix_act, mix_slope = silu_parts(mix_gate)
    mix_hidden = (mix_act * mix_up).astype(jnp.bfloat16)
    mix_back = jnp.dot(cotangent, shared_down, preferred_element_type=jnp.float32)
    mixgrad_gate = (mix_back * mix_up * mix_slope).astype(jnp.bfloat16)
    mixgrad_up = (mix_back * mix_act).astype(jnp.bfloat16)
    mix_block = FS // N_TP
    mix_input = jnp.zeros((TOKENS, row_width), jnp.float32)
    for block_index in range(N_TP):
        start_col = block_index * mix_block
        stop_col = start_col + mix_block
        partial_value = contract_cols(mixgrad_gate[:, start_col:stop_col], shared_gate[:, start_col:stop_col])
        partial_value = partial_value + contract_cols(mixgrad_up[:, start_col:stop_col], shared_up[:, start_col:stop_col])
        mix_input = mix_input + rounded(partial_value)
    token_grad = (mix_input + input_acc).astype(jnp.bfloat16)
    weight_grad = weight_acc.reshape(TOKENS, TOP_K) / route_weights
    sharedgate_grad = contract_rows(tokens, mixgrad_gate)
    sharedup_grad = contract_rows(tokens, mixgrad_up)
    shareddown_grad = contract_rows(cotangent, mix_hidden)
    return (token_grad, weight_grad, gate_grad, up_grad, down_grad, sharedgate_grad, sharedup_grad, shareddown_grad)
```

```python
import functools

import jax
import jax.numpy as jnp
from jax import lax
from jax.experimental import pallas as pl
from jax.experimental.pallas import tpu as pltpu
from jax.sharding import PartitionSpec as P

MESH = pl.DeviceIdType.MESH
F32 = jnp.float32
BF16 = jnp.bfloat16


def remote(src, dst, send, recv, device):
    return pltpu.make_async_remote_copy(
        src_ref=src,
        dst_ref=dst,
        send_sem=send,
        recv_sem=recv,
        device_id=device,
        device_id_type=MESH,
    )


def silu_parts(preact):
    sigmoid_v = jax.nn.sigmoid(preact)
    return (preact * sigmoid_v, sigmoid_v * (1.0 + preact * (1.0 - sigmoid_v)))


def dot_nn(left, right):
    return lax.dot_general(left, right, (((1,), (0,)), ((), ())), preferred_element_type=F32)


def dot_nt(left, right):
    return lax.dot_general(left, right, (((1,), (1,)), ((), ())), preferred_element_type=F32)


def dot_tn(left, right):
    return lax.dot_general(left, right, (((0,), (0,)), ((), ())), preferred_element_type=F32)


def loop(first, last, body):
    def step(s, carry):
        body(s)
        return carry

    lax.fori_loop(first, last, step, 0)


def greet(groups, me, half):
    barrier = pltpu.get_barrier_semaphore()

    def hello(s):
        pl.semaphore_signal(
            barrier, inc=1, device_id=(lax.rem(me + s, groups), half), device_id_type=MESH
        )

    loop(1, groups, hello)
    pl.semaphore_signal(barrier, inc=1, device_id=(me, 1 - half), device_id_type=MESH)
    pl.semaphore_wait(barrier, groups)


def dispatch_kernel(
    groups,
    inner,
    both,
    packed,
    cut,
    sgate,
    sup,
    sdown,
    got,
    mix_out,
    grad_gate,
    grad_up,
    grad_down,
    whole,
    cut_all,
    mixed,
    mix_part,
    mix_in,
    part,
    part_in,
    pair_sem,
    mixp_sem,
    own_sem,
    out_sem,
    in_sem,
    fwd_out_sem,
    fwd_in_sem,
    cut_sem,
    mixed_sem,
    part_sem,
):
    me = lax.axis_index("ep")
    half = lax.axis_index("tp")
    other = 1 - half
    outer = groups // inner
    slow = me // inner
    fast = me % inner
    cols = both.shape[2]
    hid = sgate.shape[1]
    cut_cols = cut.shape[3]
    mine = pl.ds(pl.multiple_of(half * cols, cols), cols)
    theirs = pl.ds(pl.multiple_of(other * cols, cols), cols)
    cut_mine = pl.ds(pl.multiple_of(half * cut_cols, cut_cols), cut_cols)
    cut_theirs = pl.ds(pl.multiple_of(other * cut_cols, cut_cols), cut_cols)
    partner = (me, other)

    greet(groups, me, half)

    pair = remote(both, whole.at[:, :, mine], pair_sem.at[0], pair_sem.at[1], partner)
    pair.start()
    own_whole = pltpu.make_async_copy(both, whole.at[:, :, mine], own_sem.at[0])
    own_whole.start()

    def member(step):
        to = (fast + step) % inner
        return to, (slow * inner + to, half)

    def source(step):
        return (fast + inner - step) % inner

    for step in range(1, inner):
        to, device = member(step)
        remote(
            cut.at[:, to],
            cut_all.at[:, fast, :, cut_mine],
            cut_sem.at[0, to],
            cut_sem.at[1, fast],
            device,
        ).start()
    own_cut = pltpu.make_async_copy(
        cut.at[:, fast], cut_all.at[:, fast, :, cut_mine], own_sem.at[1]
    )
    own_cut.start()
    remote(
        cut.at[:, fast],
        cut_all.at[:, fast, :, cut_mine],
        cut_sem.at[2, fast],
        cut_sem.at[3, fast],
        partner,
    ).start()

    own_slot = pltpu.make_async_copy(packed.at[:, me], got.at[:, me, :, mine], own_sem.at[2])
    own_slot.start()
    remote(
        packed.at[:, me], got.at[:, me, :, mine], fwd_out_sem.at[me], fwd_in_sem.at[me], partner
    ).start()

    def send_slots(s):
        to = lax.rem(me + s, groups)
        remote(
            packed.at[:, to], got.at[:, me, :, mine], out_sem.at[to], in_sem.at[me], (to, half)
        ).start()

    middle = groups // 2
    loop(1, middle, send_slots)

    own_whole.wait()
    remote(both, whole.at[:, :, theirs], pair_sem.at[0], pair_sem.at[1], partner).wait()

    rows = whole[0]
    mix_gate = dot_nn(rows, sgate[...])
    mix_up = dot_nn(rows, sup[...])
    mix_back = dot_nn(whole[1], sdown[...])
    act, slope = silu_parts(mix_gate)
    low_gate = (mix_back * mix_up * slope).astype(BF16)
    low_up = (mix_back * act).astype(BF16)
    mixed[fast, :, 0:hid] = low_gate
    mixed[fast, :, hid : 2 * hid] = low_up
    mixed[fast, :, 2 * hid : 3 * hid] = (act * mix_up).astype(BF16)

    for step in range(1, inner):
        to, device = member(step)
        remote(
            mixed.at[fast], mixed.at[fast], mixed_sem.at[0, to], mixed_sem.at[1, fast], device
        ).start()

    loop(middle, groups, send_slots)

    for piece in range(2):
        at = pl.ds(piece * cols, cols)
        mix_part[piece] = (
            dot_nt(low_gate, sgate[at, :]) + dot_nt(low_up, sup[at, :])
        ).astype(BF16)
    mixp = remote(mix_part.at[other], mix_in, mixp_sem.at[0], mixp_sem.at[1], partner)
    mixp.start()

    own_cut.wait()
    for step in range(1, inner):
        frm = source(step)
        here = cut_all.at[:, frm, :, cut_mine]
        remote(
            cut.at[:, frm], here, cut_sem.at[0, frm], cut_sem.at[1, frm], partner
        ).wait_recv()
        remote(here, here, cut_sem.at[2, frm], cut_sem.at[3, frm], partner).start()

    mixp.wait()
    mix_out[...] = mix_part[half].astype(F32) + mix_in[...].astype(F32)

    for step in range(inner):
        frm = source(step)
        here = cut_all.at[:, frm, :, cut_mine]
        there = cut_all.at[:, frm, :, cut_theirs]
        remote(here, there, cut_sem.at[2, frm], cut_sem.at[3, frm], partner).wait()
        if step > 0:
            to, device = member(step)
            remote(
                cut.at[:, to], here, cut_sem.at[0, to], cut_sem.at[1, to], device
            ).wait_send()
            remote(
                mixed.at[fast], mixed.at[frm], mixed_sem.at[0, to], mixed_sem.at[1, frm], device
            ).wait()

    depth = inner * cut.shape[2]
    wide = 2 * cut_cols
    every = mixed[...].reshape(depth, 3 * hid)
    block = part.shape[1]
    part[:, :, 0 : 2 * hid] = (
        dot_tn(cut_all[0].reshape(depth, wide), every[:, 0 : 2 * hid])
        .astype(BF16)
        .reshape(outer, block, 2 * hid)
    )
    part[:, :, 2 * hid : 3 * hid] = (
        dot_tn(cut_all[1].reshape(depth, wide), every[:, 2 * hid : 3 * hid])
        .astype(BF16)
        .reshape(outer, block, hid)
    )

    def send_part(s):
        to = lax.rem(slow + s, outer)
        remote(
            part.at[to],
            part_in.at[slow],
            part_sem.at[0, to],
            part_sem.at[1, slow],
            (to * inner + fast, half),
        ).start()

    loop(1, outer, send_part)

    def forward(s):
        frm = lax.rem(me + groups - s, groups)
        here = got.at[:, frm, :, mine]
        remote(packed.at[:, frm], here, out_sem.at[frm], in_sem.at[frm], partner).wait_recv()
        remote(here, here, fwd_out_sem.at[frm], fwd_in_sem.at[frm], partner).start()

    loop(1, groups, forward)

    total = part[slow].astype(F32)
    grad_gate[...] = total[:, 0:hid]
    grad_up[...] = total[:, hid : 2 * hid]
    grad_down[...] = total[:, 2 * hid : 3 * hid]

    def take_part(s):
        frm = lax.rem(slow + outer - s, outer)
        remote(
            part.at[frm], part_in.at[frm], part_sem.at[0, frm], part_sem.at[1, frm], partner
        ).wait()
        term = part_in[frm].astype(F32)
        grad_gate[...] += term[:, 0:hid]
        grad_up[...] += term[:, hid : 2 * hid]
        grad_down[...] += term[:, 2 * hid : 3 * hid]

    loop(1, outer, take_part)

    own_slot.wait()

    def finish(s):
        frm = lax.rem(me + groups - s, groups)
        here = got.at[:, frm, :, mine]
        there = got.at[:, frm, :, theirs]
        remote(here, there, fwd_out_sem.at[frm], fwd_in_sem.at[frm], partner).wait()

    loop(0, groups, finish)

    def sent(s):
        to = lax.rem(me + s, groups)
        here = got.at[:, to, :, mine]
        remote(packed.at[:, to], here, out_sem.at[to], in_sem.at[to], partner).wait_send()

    loop(1, groups, sent)


def dispatch(groups, inner, both, packed, cut, sgate, sup, sdown):
    _, token_rows, cols = both.shape
    per_peer = packed.shape[2]
    width = 2 * cols
    hid = sgate.shape[1]
    outer = groups // inner
    block = width // groups
    vmem = pl.BlockSpec(memory_space=pltpu.VMEM)
    grad = jax.ShapeDtypeStruct((block, hid), F32)
    dma = pltpu.SemaphoreType.DMA
    return pl.pallas_call(
        functools.partial(dispatch_kernel, groups, inner),
        out_shape=(
            jax.ShapeDtypeStruct((2, groups, per_peer, width), BF16),
            jax.ShapeDtypeStruct((token_rows, cols), F32),
            grad,
            grad,
            grad,
        ),
        in_specs=[vmem] * 6,
        out_specs=(pl.BlockSpec(memory_space=pl.ANY), vmem, vmem, vmem, vmem),
        scratch_shapes=[
            pltpu.VMEM((2, token_rows, width), BF16),
            pltpu.VMEM((2, inner, token_rows, width // inner), BF16),
            pltpu.VMEM((inner, token_rows, 3 * hid), BF16),
            pltpu.VMEM((2, token_rows, cols), BF16),
            pltpu.VMEM((token_rows, cols), BF16),
            pltpu.VMEM((outer, block, 3 * hid), BF16),
            pltpu.VMEM((outer, block, 3 * hid), BF16),
            dma((2,)),
            dma((2,)),
            dma((3,)),
            dma((groups,)),
            dma((groups,)),
            dma((groups,)),
            dma((groups,)),
            dma((4, inner)),
            dma((2, inner)),
            dma((2, outer)),
        ],
        compiler_params=pltpu.CompilerParams(collective_id=0, has_side_effects=True),
        name="dispatch",
    )(both, packed, cut, sgate, sup, sdown)


def home_kernel(groups, terms, home, taken, back, pair_sem, own_sem, out_sem, in_sem):
    me = lax.axis_index("ep")
    half = lax.axis_index("tp")
    other = 1 - half
    greet(groups, me, half)
    pair = remote(terms.at[other], taken, pair_sem.at[0], pair_sem.at[1], (me, other))
    pair.start()
    pair.wait()

    def add(s):
        back[s] = (terms[half, s].astype(F32) + taken[s].astype(F32)).astype(BF16)

    loop(0, groups, add)
    own = pltpu.make_async_copy(back.at[me], home.at[me], own_sem)
    own.start()

    def send(s):
        to = lax.rem(me + s, groups)
        remote(back.at[to], home.at[me], out_sem.at[to], in_sem.at[me], (to, half)).start()

    loop(1, groups, send)
    own.wait()

    def take(s):
        frm = lax.rem(me + groups - s, groups)
        remote(back.at[frm], home.at[frm], out_sem.at[frm], in_sem.at[frm], (frm, half)).wait()

    loop(1, groups, take)


def send_home(groups, terms):
    shape = terms.shape[1:]
    vmem = pl.BlockSpec(memory_space=pltpu.VMEM)
    dma = pltpu.SemaphoreType.DMA
    return pl.pallas_call(
        functools.partial(home_kernel, groups),
        out_shape=jax.ShapeDtypeStruct(shape, BF16),
        in_specs=[vmem],
        out_specs=pl.BlockSpec(memory_space=pl.ANY),
        scratch_shapes=[
            pltpu.VMEM(shape, BF16),
            pltpu.VMEM(shape, BF16),
            dma((2,)),
            dma,
            dma((groups,)),
            dma((groups,)),
        ],
        compiler_params=pltpu.CompilerParams(collective_id=1, has_side_effects=True),
        name="home",
    )(terms)


def per_device(
    tokens,
    cotangent,
    routes,
    route_weights,
    gate_proj,
    up_proj,
    down_proj,
    shared_gate,
    shared_up,
    shared_down,
):
    groups = lax.axis_size("ep")
    halves = lax.axis_size("tp")
    local_count = gate_proj.shape[0]
    experts = groups * local_count
    token_rows, top = routes.shape
    assigned = token_rows * top
    capacity = assigned // experts + assigned // (2 * experts)
    per_peer = local_count * capacity
    slots = experts * capacity
    cols = tokens.shape[1]
    inner = 4
    outer = groups // inner
    block = halves * cols // groups

    names = routes.T
    named = (names[:, :, None] == jnp.arange(experts, dtype=jnp.int32)).astype(BF16)
    order = jnp.arange(token_rows, dtype=jnp.int32)
    earlier = (order[None, :] < order[:, None]).astype(BF16)
    before = dot_nn(earlier, named[0] + named[1])
    rank = jnp.sum(before[None] * named.astype(F32), axis=2)
    slot_of = names * capacity + rank.astype(jnp.int32)
    hit = slot_of[:, None, :] == jnp.arange(slots, dtype=jnp.int32)[None, :, None]
    chosen = (hit[0] | hit[1]).astype(BF16)
    slot_weight = jnp.sum(jnp.where(hit, route_weights.T[:, None, :], 0.0), axis=(0, 2))
    packed_rows = dot_nn(chosen, tokens).astype(BF16)
    packed_cot = (slot_weight[:, None] * dot_nn(chosen, cotangent)).astype(BF16)
    packed = jnp.stack([packed_rows, packed_cot]).reshape(2, groups, per_peer, cols)
    both = jnp.stack([tokens, cotangent])
    cut = (
        both.reshape(2, token_rows, outer // halves, inner, block)
        .transpose(0, 3, 1, 2, 4)
        .reshape(2, inner, token_rows, cols // inner)
    )
    got, mix_sum, sharedgate_grad, sharedup_grad, shareddown_grad = dispatch(
        groups, inner, both, packed, cut, shared_gate, shared_up, shared_down
    )

    def by_expert(layout):
        return jnp.swapaxes(layout.reshape(groups, local_count, capacity, -1), 0, 1).reshape(
            local_count, groups * capacity, -1
        )

    def by_peer(layout):
        return jnp.swapaxes(layout.reshape(local_count, groups, capacity, -1), 0, 1).reshape(
            groups, per_peer, -1
        )

    slot_rows = by_expert(got[0])
    slot_cot = by_expert(got[1])
    gate_pre = jnp.einsum("erd,edf->erf", slot_rows, gate_proj, preferred_element_type=F32)
    up_pre = jnp.einsum("erd,edf->erf", slot_rows, up_proj, preferred_element_type=F32)
    gate_act, gate_slope = silu_parts(gate_pre)
    hidden = gate_act * up_pre
    back_grad = jnp.einsum("erd,efd->erf", slot_cot, down_proj, preferred_element_type=F32)
    product = jnp.sum(hidden * back_grad, axis=2, keepdims=True)
    hidden_low = hidden.astype(BF16)
    gate_delta = (back_grad * up_pre * gate_slope).astype(BF16)
    up_delta = (back_grad * gate_act).astype(BF16)
    input_part = jnp.einsum("erf,edf->erd", gate_delta, gate_proj, preferred_element_type=F32)
    input_part = input_part + jnp.einsum(
        "erf,edf->erd", up_delta, up_proj, preferred_element_type=F32
    )
    sent_part = by_peer(input_part.astype(BF16))
    lanes = jnp.broadcast_to(by_peer(product.astype(BF16)), (groups, per_peer, 128))
    terms = jnp.stack(
        [
            jnp.concatenate([sent_part[:, :, h * cols : (h + 1) * cols], lanes], axis=2)
            for h in range(halves)
        ]
    )
    home = send_home(groups, terms).reshape(slots, cols + 128)

    down_grad = jnp.einsum("erf,erd->efd", hidden_low, slot_cot, preferred_element_type=F32)
    gate_grad = jnp.einsum("erd,erf->edf", slot_rows, gate_delta, preferred_element_type=F32)
    up_grad = jnp.einsum("erd,erf->edf", slot_rows, up_delta, preferred_element_type=F32)

    token_grad = (mix_sum + dot_tn(chosen, home[:, :cols])).astype(BF16)
    slot_product = home[:, cols].astype(F32)
    weight_grad = (
        jnp.sum(jnp.where(hit, slot_product[None, :, None], 0.0), axis=1).T / route_weights
    )
    return (
        token_grad,
        weight_grad,
        gate_grad.astype(BF16),
        up_grad.astype(BF16),
        down_grad.astype(BF16),
        sharedgate_grad,
        sharedup_grad,
        shareddown_grad,
    )


def solution(mesh):
    in_specs = (
        P("ep", "tp"),
        P("ep", "tp"),
        P("ep", None),
        P("ep", None),
        P("ep", None, "tp"),
        P("ep", None, "tp"),
        P("ep", "tp", None),
        P(None, "tp"),
        P(None, "tp"),
        P(None, "tp"),
    )
    out_specs = (
        P("ep", "tp"),
        P("ep", None),
        P("ep", None, "tp"),
        P("ep", None, "tp"),
        P("ep", "tp", None),
        P("ep", "tp"),
        P("ep", "tp"),
        P("ep", "tp"),
    )
    return jax.shard_map(
        per_device, mesh=mesh, in_specs=in_specs, out_specs=out_specs, check_vma=False
    )
```

```python
import functools

import jax
import jax.numpy as jnp
from jax import lax
from jax.experimental import pallas as pl
from jax.experimental.pallas import tpu as pltpu
from jax.sharding import PartitionSpec as P

MESH = pl.DeviceIdType.MESH
F32 = jnp.float32
BF16 = jnp.bfloat16


def remote(src, dst, send, recv, device):
    return pltpu.make_async_remote_copy(
        src_ref=src,
        dst_ref=dst,
        send_sem=send,
        recv_sem=recv,
        device_id=device,
        device_id_type=MESH,
    )


def silu_parts(preact):
    sigmoid_v = jax.nn.sigmoid(preact)
    return (preact * sigmoid_v, sigmoid_v * (1.0 + preact * (1.0 - sigmoid_v)))


def dot_nn(left, right):
    return lax.dot_general(left, right, (((1,), (0,)), ((), ())), preferred_element_type=F32)


def dot_nt(left, right):
    return lax.dot_general(left, right, (((1,), (1,)), ((), ())), preferred_element_type=F32)


def dot_tn(left, right):
    return lax.dot_general(left, right, (((0,), (0,)), ((), ())), preferred_element_type=F32)


def loop(first, last, body):
    def step(s, carry):
        body(s)
        return carry

    lax.fori_loop(first, last, step, 0)


def greet(groups, me, half):
    barrier = pltpu.get_barrier_semaphore()

    def hello(s):
        pl.semaphore_signal(
            barrier, inc=1, device_id=(lax.rem(me + s, groups), half), device_id_type=MESH
        )

    loop(1, groups, hello)
    pl.semaphore_signal(barrier, inc=1, device_id=(me, 1 - half), device_id_type=MESH)
    pl.semaphore_wait(barrier, groups)


def dispatch_kernel(
    groups,
    inner,
    tok,
    cot,
    packed_rows,
    packed_cot,
    sgate,
    sup,
    sdown,
    got_rows,
    got_cot,
    mix_out,
    grad_gate,
    grad_up,
    grad_down,
    whole,
    cut,
    cut_all,
    mixed,
    mix_part,
    mix_in,
    part,
    part_in,
    pair_sem,
    mixp_sem,
    own_sem,
    out_sem,
    in_sem,
    fwd_out_sem,
    fwd_in_sem,
    cut_sem,
    mixed_sem,
    part_sem,
):
    me = lax.axis_index("ep")
    half = lax.axis_index("tp")
    other = 1 - half
    outer = groups // inner
    slow = me // inner
    fast = me % inner
    cols = tok.shape[1]
    width = 2 * cols
    block = width // groups
    packed = (packed_rows, packed_cot)
    got = (got_rows, got_cot)
    hid = sgate.shape[1]
    cut_cols = cut.shape[3]
    mine = pl.ds(pl.multiple_of(half * cols, cols), cols)
    theirs = pl.ds(pl.multiple_of(other * cols, cols), cols)
    cut_mine = pl.ds(pl.multiple_of(half * cut_cols, cut_cols), cut_cols)
    cut_theirs = pl.ds(pl.multiple_of(other * cut_cols, cut_cols), cut_cols)
    partner = (me, other)

    for to in range(inner):
        for piece in range(outer // 2):
            frm = pl.ds((piece * inner + to) * block, block)
            at = pl.ds(piece * block, block)
            cut[0, to, :, at] = tok[:, frm]
            cut[1, to, :, at] = cot[:, frm]

    greet(groups, me, half)

    def own_whole(i):
        return pltpu.make_async_copy((tok, cot)[i], whole.at[i, :, mine], own_sem.at[i])

    def pair(i, at):
        return remote(
            (tok, cot)[i], whole.at[i, :, at], pair_sem.at[0, i], pair_sem.at[1, i], partner
        )

    for i in range(2):
        pair(i, mine).start()
        own_whole(i).start()

    def member(step):
        to = (fast + step) % inner
        return to, (slow * inner + to, half)

    def source(step):
        return (fast + inner - step) % inner

    for step in range(1, inner):
        to, device = member(step)
        remote(
            cut.at[:, to],
            cut_all.at[:, fast, :, cut_mine],
            cut_sem.at[0, to],
            cut_sem.at[1, fast],
            device,
        ).start()
    own_cut = pltpu.make_async_copy(
        cut.at[:, fast], cut_all.at[:, fast, :, cut_mine], own_sem.at[2]
    )
    own_cut.start()
    remote(
        cut.at[:, fast],
        cut_all.at[:, fast, :, cut_mine],
        cut_sem.at[2, fast],
        cut_sem.at[3, fast],
        partner,
    ).start()

    def out_copy(i, to, frm, device):
        return remote(
            packed[i].at[to],
            got[i].at[frm, :, mine],
            out_sem.at[i, to],
            in_sem.at[i, frm],
            device,
        )

    def forward_copy(i, frm, at):
        here = got[i].at[frm, :, at]
        return remote(here, here, fwd_out_sem.at[i, frm], fwd_in_sem.at[i, frm], partner)

    def own_slot(i):
        return pltpu.make_async_copy(
            packed[i].at[me], got[i].at[me, :, mine], own_sem.at[3 + i]
        )

    def over(di, first, body):
        loop(first, outer, lambda do: body(do, di))

    def send_slots(do, di):
        to = lax.rem(slow + do, outer) * inner + lax.rem(fast + di, inner)
        for i in range(2):
            out_copy(i, to, me, (to, half)).start()

    over(0, 1, send_slots)

    for i in range(2):
        own_whole(i).wait()
        pair(i, theirs).wait()

    rows = whole[0]
    mix_gate = dot_nn(rows, sgate[...])
    mix_up = dot_nn(rows, sup[...])
    mix_back = dot_nn(whole[1], sdown[...])
    act, slope = silu_parts(mix_gate)
    low_gate = (mix_back * mix_up * slope).astype(BF16)
    low_up = (mix_back * act).astype(BF16)
    mixed[fast, :, 0:hid] = low_gate
    mixed[fast, :, hid : 2 * hid] = low_up
    mixed[fast, :, 2 * hid : 3 * hid] = (act * mix_up).astype(BF16)

    for step in range(1, inner):
        to, device = member(step)
        remote(
            mixed.at[fast], mixed.at[fast], mixed_sem.at[0, to], mixed_sem.at[1, fast], device
        ).start()

    over(1, 1, send_slots)

    for piece in range(2):
        at = pl.ds(piece * cols, cols)
        mix_part[piece] = (
            dot_nt(low_gate, sgate[at, :]) + dot_nt(low_up, sup[at, :])
        ).astype(BF16)
    mixp = remote(mix_part.at[other], mix_in, mixp_sem.at[0], mixp_sem.at[1], partner)
    mixp.start()

    own_cut.wait()
    for step in range(1, inner):
        frm = source(step)
        here = cut_all.at[:, frm, :, cut_mine]
        remote(
            cut.at[:, frm], here, cut_sem.at[0, frm], cut_sem.at[1, frm], partner
        ).wait_recv()
        remote(here, here, cut_sem.at[2, frm], cut_sem.at[3, frm], partner).start()

    mixp.wait()
    mix_out[...] = mix_part[half].astype(F32) + mix_in[...].astype(F32)

    for step in range(inner):
        frm = source(step)
        here = cut_all.at[:, frm, :, cut_mine]
        there = cut_all.at[:, frm, :, cut_theirs]
        remote(here, there, cut_sem.at[2, frm], cut_sem.at[3, frm], partner).wait()
        if step > 0:
            to, device = member(step)
            remote(
                cut.at[:, to], here, cut_sem.at[0, to], cut_sem.at[1, to], device
            ).wait_send()
            remote(
                mixed.at[fast], mixed.at[frm], mixed_sem.at[0, to], mixed_sem.at[1, frm], device
            ).wait()

    depth = inner * cut.shape[2]
    wide = 2 * cut_cols
    every = mixed[...].reshape(depth, 3 * hid)
    part[:, :, 0 : 2 * hid] = (
        dot_tn(cut_all[0].reshape(depth, wide), every[:, 0 : 2 * hid])
        .astype(BF16)
        .reshape(outer, block, 2 * hid)
    )
    part[:, :, 2 * hid : 3 * hid] = (
        dot_tn(cut_all[1].reshape(depth, wide), every[:, 2 * hid : 3 * hid])
        .astype(BF16)
        .reshape(outer, block, hid)
    )

    def exchange(stride, first):
        bit = (slow // stride) % 2
        low = slow % stride
        keep = low + bit * stride
        give = low + (1 - bit) * stride
        device = ((slow + stride - 2 * bit * stride) * inner + fast, half)
        count = outer // (2 * stride)

        def copy(n):
            return remote(
                part.at[give + 2 * stride * n],
                part_in.at[first + n],
                part_sem.at[0, first + n],
                part_sem.at[1, first + n],
                device,
            )

        def start():
            loop(0, count, lambda n: copy(n).start())

        def finish():
            loop(0, count, lambda n: copy(n).wait())

        def merged(n):
            return part[keep + 2 * stride * n].astype(F32) + part_in[first + n].astype(F32)

        def fold():
            def one(n):
                part[keep + 2 * stride * n] = merged(n).astype(BF16)

            loop(0, count, one)

        return start, finish, merged, fold, count

    stride, first = 1, 0
    rest = [(di, 1) for di in range(2, inner)] + [(di, 0) for di in range(1, inner)]
    while stride < outer:
        start, finish, merged, fold, count = exchange(stride, first)
        start()
        if stride * 2 >= outer:
            for di, do in rest:
                loop(do, outer if do else 1, lambda do, di=di: send_slots(do, di))
        elif rest and rest[0][1]:
            over(rest[0][0], 1, send_slots)
            rest = rest[1:]
        if stride * 2 < outer:
            finish()
            fold()
        first += count
        stride *= 2

    def forward(do, di):
        frm = lax.rem(slow + outer - do, outer) * inner + lax.rem(fast + inner - di, inner)
        for i in range(2):
            out_copy(i, frm, frm, partner).wait_recv()
            forward_copy(i, frm, mine).start()

    for i in range(2):
        own_slot(i).start()
        remote(
            packed[i].at[me],
            got[i].at[me, :, mine],
            fwd_out_sem.at[i, me],
            fwd_in_sem.at[i, me],
            partner,
        ).start()
    over(0, 1, forward)
    over(1, 1, forward)
    over(2, 1, forward)

    finish()
    total = merged(0)
    grad_gate[...] = total[:, 0:hid]
    grad_up[...] = total[:, hid : 2 * hid]
    grad_down[...] = total[:, 2 * hid : 3 * hid]

    for di in range(1, inner):
        loop(0, 1, lambda do, di=di: forward(do, di))
    for di in range(3, inner):
        over(di, 1, forward)

    def drain(s):
        frm = lax.rem(me + groups - s, groups)
        for i in range(2):
            forward_copy(i, frm, mine).wait_send()
            forward_copy(i, frm, theirs).wait_recv()

    loop(0, groups, drain)
    for i in range(2):
        own_slot(i).wait()

    def sent(s):
        to = lax.rem(me + s, groups)
        for i in range(2):
            out_copy(i, to, to, partner).wait_send()

    loop(1, groups, sent)


def dispatch(groups, inner, tok, cot, packed_rows, packed_cot, sgate, sup, sdown):
    token_rows, cols = tok.shape
    per_peer = packed_rows.shape[1]
    width = 2 * cols
    hid = sgate.shape[1]
    outer = groups // inner
    block = width // groups
    vmem = pl.BlockSpec(memory_space=pltpu.VMEM)
    anyspace = pl.BlockSpec(memory_space=pl.ANY)
    slots = jax.ShapeDtypeStruct((groups, per_peer, width), BF16)
    grad = jax.ShapeDtypeStruct((block, hid), F32)
    dma = pltpu.SemaphoreType.DMA
    return pl.pallas_call(
        functools.partial(dispatch_kernel, groups, inner),
        out_shape=(
            slots,
            slots,
            jax.ShapeDtypeStruct((token_rows, cols), F32),
            grad,
            grad,
            grad,
        ),
        in_specs=[vmem] * 7,
        out_specs=(anyspace, anyspace, vmem, vmem, vmem, vmem),
        scratch_shapes=[
            pltpu.VMEM((2, token_rows, width), BF16),
            pltpu.VMEM((2, inner, token_rows, cols // inner), BF16),
            pltpu.VMEM((2, inner, token_rows, width // inner), BF16),
            pltpu.VMEM((inner, token_rows, 3 * hid), BF16),
            pltpu.VMEM((2, token_rows, cols), BF16),
            pltpu.VMEM((token_rows, cols), BF16),
            pltpu.VMEM((outer, block, 3 * hid), BF16),
            pltpu.VMEM((outer, block, 3 * hid), BF16),
            dma((2, 2)),
            dma((2,)),
            dma((5,)),
            dma((2, groups)),
            dma((2, groups)),
            dma((2, groups)),
            dma((2, groups)),
            dma((4, inner)),
            dma((2, inner)),
            dma((2, outer)),
        ],
        compiler_params=pltpu.CompilerParams(collective_id=0, has_side_effects=True),
        name="dispatch",
    )(tok, cot, packed_rows, packed_cot, sgate, sup, sdown)


def home_kernel(groups, terms, lanes, home, taken, back, pair_sem, own_sem, out_sem, in_sem):
    me = lax.axis_index("ep")
    half = lax.axis_index("tp")
    other = 1 - half
    greet(groups, me, half)
    wide, cols = lanes.shape[2], terms.shape[2] // 2
    mine = pl.ds(pl.multiple_of(half * cols, cols), cols)
    theirs = pl.ds(pl.multiple_of(other * cols, cols), cols)
    main, tail = pl.ds(0, cols), pl.ds(cols, wide)
    partner = (me, other)
    pair = remote(
        terms.at[:, :, theirs], taken.at[:, :, main], pair_sem.at[0, 0], pair_sem.at[1, 0], partner
    )
    side = remote(lanes, taken.at[:, :, tail], pair_sem.at[0, 1], pair_sem.at[1, 1], partner)
    pair.start()
    side.start()
    pair.wait()
    side.wait()

    def add(s):
        back[s, :, main] = (terms[s, :, mine].astype(F32) + taken[s, :, main].astype(F32)).astype(
            BF16
        )
        back[s, :, tail] = (lanes[s].astype(F32) + taken[s, :, tail].astype(F32)).astype(BF16)

    loop(0, groups, add)
    own = pltpu.make_async_copy(back.at[me], home.at[me], own_sem)
    own.start()

    def send(s):
        to = lax.rem(me + s, groups)
        remote(back.at[to], home.at[me], out_sem.at[to], in_sem.at[me], (to, half)).start()

    loop(1, groups, send)
    own.wait()

    def take(s):
        frm = lax.rem(me + groups - s, groups)
        remote(back.at[frm], home.at[frm], out_sem.at[frm], in_sem.at[frm], (frm, half)).wait()

    loop(1, groups, take)


def send_home(groups, terms, lanes):
    shape = (*terms.shape[:2], terms.shape[2] // 2 + lanes.shape[2])
    vmem = pl.BlockSpec(memory_space=pltpu.VMEM)
    dma = pltpu.SemaphoreType.DMA
    return pl.pallas_call(
        functools.partial(home_kernel, groups),
        out_shape=jax.ShapeDtypeStruct(shape, BF16),
        in_specs=[vmem, vmem],
        out_specs=pl.BlockSpec(memory_space=pl.ANY),
        scratch_shapes=[
            pltpu.VMEM(shape, BF16),
            pltpu.VMEM(shape, BF16),
            dma((2, 2)),
            dma,
            dma((groups,)),
            dma((groups,)),
        ],
        compiler_params=pltpu.CompilerParams(collective_id=1, has_side_effects=True),
        name="home",
    )(terms, lanes)


def per_device(
    tokens,
    cotangent,
    routes,
    route_weights,
    gate_proj,
    up_proj,
    down_proj,
    shared_gate,
    shared_up,
    shared_down,
):
    groups = lax.axis_size("ep")
    local_count = gate_proj.shape[0]
    experts = groups * local_count
    token_rows, top = routes.shape
    assigned = token_rows * top
    capacity = assigned // experts + assigned // (2 * experts)
    per_peer = local_count * capacity
    slots = experts * capacity
    cols = tokens.shape[1]
    inner = 4

    names = routes.T
    named = (names[:, :, None] == jnp.arange(experts, dtype=jnp.int32)).astype(BF16)
    order = jnp.arange(token_rows, dtype=jnp.int32)
    earlier = (order[None, :] < order[:, None]).astype(BF16)
    before = dot_nn(earlier, named[0] + named[1])
    rank = jnp.sum(before[None] * named.astype(F32), axis=2)
    slot_of = names * capacity + rank.astype(jnp.int32)
    hit = slot_of[:, None, :] == jnp.arange(slots, dtype=jnp.int32)[None, :, None]
    chosen = (hit[0] | hit[1]).astype(BF16)
    slot_weight = jnp.sum(jnp.where(hit, route_weights.T[:, None, :], 0.0), axis=(0, 2))
    packed_rows = dot_nn(chosen, tokens).astype(BF16)
    packed_cot = (slot_weight[:, None] * dot_nn(chosen, cotangent)).astype(BF16)
    got_rows, got_cot, mix_sum, sharedgate_grad, sharedup_grad, shareddown_grad = dispatch(
        groups,
        inner,
        tokens,
        cotangent,
        packed_rows.reshape(groups, per_peer, cols),
        packed_cot.reshape(groups, per_peer, cols),
        shared_gate,
        shared_up,
        shared_down,
    )

    def by_expert(layout):
        return jnp.swapaxes(layout.reshape(groups, local_count, capacity, -1), 0, 1).reshape(
            local_count, groups * capacity, -1
        )

    def by_peer(layout):
        return jnp.swapaxes(layout.reshape(local_count, groups, capacity, -1), 0, 1).reshape(
            groups, per_peer, -1
        )

    slot_rows = by_expert(got_rows)
    slot_cot = by_expert(got_cot)
    gate_pre = jnp.einsum("erd,edf->erf", slot_rows, gate_proj, preferred_element_type=F32)
    up_pre = jnp.einsum("erd,edf->erf", slot_rows, up_proj, preferred_element_type=F32)
    gate_act, gate_slope = silu_parts(gate_pre)
    hidden = gate_act * up_pre
    back_grad = jnp.einsum("erd,efd->erf", slot_cot, down_proj, preferred_element_type=F32)
    product = jnp.sum(hidden * back_grad, axis=2, keepdims=True)
    hidden_low = hidden.astype(BF16)
    gate_delta = (back_grad * up_pre * gate_slope).astype(BF16)
    up_delta = (back_grad * gate_act).astype(BF16)
    input_part = jnp.einsum("erf,edf->erd", gate_delta, gate_proj, preferred_element_type=F32)
    input_part = input_part + jnp.einsum(
        "erf,edf->erd", up_delta, up_proj, preferred_element_type=F32
    )
    sent_part = by_peer(input_part.astype(BF16))
    lanes = jnp.broadcast_to(by_peer(product.astype(BF16)), (groups, per_peer, 128))
    home = send_home(groups, sent_part, lanes).reshape(slots, cols + 128)

    down_grad = jnp.einsum("erf,erd->efd", hidden_low, slot_cot, preferred_element_type=F32)
    gate_grad = jnp.einsum("erd,erf->edf", slot_rows, gate_delta, preferred_element_type=F32)
    up_grad = jnp.einsum("erd,erf->edf", slot_rows, up_delta, preferred_element_type=F32)

    token_grad = (mix_sum + dot_tn(chosen, home[:, :cols])).astype(BF16)
    slot_product = home[:, cols].astype(F32)
    weight_grad = (
        jnp.sum(jnp.where(hit, slot_product[None, :, None], 0.0), axis=1).T / route_weights
    )
    return (
        token_grad,
        weight_grad,
        gate_grad.astype(BF16),
        up_grad.astype(BF16),
        down_grad.astype(BF16),
        sharedgate_grad,
        sharedup_grad,
        shareddown_grad,
    )


def solution(mesh):
    in_specs = (
        P("ep", "tp"),
        P("ep", "tp"),
        P("ep", None),
        P("ep", None),
        P("ep", None, "tp"),
        P("ep", None, "tp"),
        P("ep", "tp", None),
        P(None, "tp"),
        P(None, "tp"),
        P(None, "tp"),
    )
    out_specs = (
        P("ep", "tp"),
        P("ep", None),
        P("ep", None, "tp"),
        P("ep", None, "tp"),
        P("ep", "tp", None),
        P("ep", "tp"),
        P("ep", "tp"),
        P("ep", "tp"),
    )
    return jax.shard_map(
        per_device, mesh=mesh, in_specs=in_specs, out_specs=out_specs, check_vma=False
    )
```
